32 devices in a mesh: rep: 2 (over x), fs: 4 (over z), tp: 4 (over y, core).
Axes of the slice: x: 2, y: 2, z: 4, core: 2. Of those that a mesh axis runs over, the one named last changes fastest.
Arguments:
- tokens: bfloat16 [4096, 2048], P(('rep', 'fs', 'tp')), may hold values from -6 to 6
- mix_gain: bfloat16 [2048], replicated, may hold values from 0.099609375 to 1.8984375
- gate_proj: bfloat16 [2048, 512], P('fs', 'tp'), may hold values from -0.125 to 0.125
- value_proj: bfloat16 [2048, 512], P('fs', 'tp'), may hold values from -1 to 1
- layer_gain: bfloat16 [512], replicated, may hold values from 0.099609375 to 1.8984375
- layer_shift: bfloat16 [512], replicated, may hold values from -3 to 3
- mix_kernel: bfloat16 [4, 128, 128], replicated, may hold values from -0.5 to 0.5
- mix_offset: bfloat16 [4, 128], replicated, may hold values from -4 to 4
- out_proj: bfloat16 [2048, 512], P('fs', 'tp'), may hold values from -0.25 to 0.25
- ffn_gain: bfloat16 [2048], replicated, may hold values from 0.099609375 to 1.8984375
- ffn_gate: bfloat16 [2048, 5632], P('fs', 'tp'), may hold values from -0.125 to 0.125
- ffn_up: bfloat16 [2048, 5632], P('fs', 'tp'), may hold values from -0.125 to 0.125
- ffn_down: bfloat16 [2048, 5632], P('fs', 'tp'), may hold values from -0.078125 to 0.078125
Outputs:
- layer_out: bfloat16 [4096, 2048], P(('rep', 'fs', 'tp'))
The draws below stay inside these ranges and needn't reach their ends.
All inputs are finite; a program needn't handle non-finite values.
Results may differ from the reference program's by a relative error of at most 0.015.
Values may be sent and summed in bfloat16 or wider, within the bound.
No kernel may reach another device: no remote copies, remote signals or barrier semaphores. Data moves between devices by JAX's collectives and lax.ppermute only.
A program may use at most 64 MiB of HBM per device.

```python
import math
import jax
import jax.numpy as jnp
from jax import lax

D = 2048
FF = 5632
W = 512
GROUP_CH = 128
BLOCK = 128
GROUPS = 4
TOKENS = 4096
N_TP = 4


def draw_value_proj(key, part):
    key_entries = jax.random.fold_in(key, 11)
    key_columns = jax.random.fold_in(key, 12)
    column_pos = jnp.arange(W, dtype=jnp.float32) / max(W - 1, 1)
    jitter = jnp.exp(jax.random.uniform(key_columns, (W,), jnp.float32, 0.0, math.log(4.0)))
    entries = jax.random.normal(key_entries, (D, W), jnp.float32)
    trend = jnp.exp(column_pos * math.log(3.0))
    scaled = entries * D ** (-0.5) * trend[None, :] * jitter[None, :]
    return jnp.clip(scaled, -1.0, 1.0).astype(jnp.bfloat16)


def block_levels(key, dims, pieces, least, high):
    def one(axis_at, shards_of):
        steps = jax.random.uniform(jax.random.fold_in(jax.random.fold_in(key, 6), axis_at), (shards_of,), jnp.float32, least / len(pieces), high / len(pieces))
        return jnp.repeat(jnp.exp(steps), dims[axis_at] // shards_of).reshape((-1,) + (1,) * (len(dims) - axis_at - 1))

    loudness = one(*pieces[0])
    for cut in pieces[1:]:
        loudness = loudness * one(*cut)
    return loudness


def normal_values(rng, dims, width, limit, pieces=(), kind=jnp.bfloat16):
    values = width * jax.random.normal(rng, dims, jnp.float32)
    if pieces:
        values = values * block_levels(rng, dims, pieces, -0.22, 0.18)
    return jnp.clip(values, -limit, limit).astype(kind)


def setup_inputs(seed: int = 0) -> dict:
    streams_of = jax.random.split(jax.random.key(seed), 14)
    tokens = normal_values(streams_of[0], (TOKENS, D), 1.0, 6.0, ((0, 32),))
    mix_gain = jnp.clip(1.0 + 0.18 * jax.random.normal(streams_of[1], (D,), jnp.float32), 0.099609375, 1.8984375).astype(jnp.bfloat16)
    gate_proj = normal_values(streams_of[2], (D, W), D ** -0.5, 0.125, ((0, 4), (1, 4)))
    value_proj = draw_value_proj(jax.random.fold_in(streams_of[13], 71), 0)
    layer_gain = jnp.clip(1.0 + 0.18 * jax.random.normal(streams_of[4], (W,), jnp.float32), 0.099609375, 1.8984375).astype(jnp.bfloat16)
    layer_shift = normal_values(streams_of[5], (W,), 0.5, 3.0)
    mix_kernel = normal_values(streams_of[6], (GROUPS, BLOCK, BLOCK), BLOCK ** -0.5, 0.5)
    mix_offset = normal_values(streams_of[7], (GROUPS, BLOCK), 1.0, 4.0)
    out_proj = normal_values(streams_of[8], (D, W), W ** -0.5, 0.25, ((0, 4), (1, 4)))
    ffn_gain = jnp.clip(1.0 + 0.18 * jax.random.normal(streams_of[9], (D,), jnp.float32), 0.099609375, 1.8984375).astype(jnp.bfloat16)
    ffn_gate = normal_values(streams_of[10], (D, FF), D ** -0.5, 0.125, ((0, 4), (1, 4)))
    ffn_up = normal_values(streams_of[11], (D, FF), D ** -0.5, 0.125, ((0, 4), (1, 4)))
    ffn_down = normal_values(streams_of[12], (D, FF), FF ** -0.5, 0.078125, ((0, 4), (1, 4)))
    return dict(tokens=tokens, mix_gain=mix_gain, gate_proj=gate_proj, value_proj=value_proj, layer_gain=layer_gain, layer_shift=layer_shift, mix_kernel=mix_kernel, mix_offset=mix_offset, out_proj=out_proj, ffn_gain=ffn_gain, ffn_gate=ffn_gate, ffn_up=ffn_up, ffn_down=ffn_down)


epsilon = 1e-06

def rms_norm(rows, gain):
    floats = rows.astype(jnp.float32)
    scale = lax.rsqrt(lax.optimization_barrier(jnp.mean(floats * floats, axis=-1, keepdims=True)) + epsilon)
    return (floats * scale * gain.astype(jnp.float32)).astype(jnp.bfloat16)

def reference(tokens, mix_gain, gate_proj, value_proj, layer_gain, layer_shift, mix_kernel, mix_offset, out_proj, ffn_gain, ffn_gate, ffn_up, ffn_down):
    normed = rms_norm(tokens, mix_gain)
    gate_u = jax.nn.gelu(jnp.dot(normed, gate_proj, preferred_element_type=jnp.float32))
    activated = jax.nn.gelu(jnp.dot(normed, value_proj, preferred_element_type=jnp.float32))
    center = lax.optimization_barrier(jnp.sum(activated, axis=-1, keepdims=True)) / W
    spread = lax.optimization_barrier(jnp.sum(activated * activated, axis=-1, keepdims=True)) / W - center * center
    values = ((activated - center) * lax.rsqrt(spread + epsilon) * layer_gain.astype(jnp.float32) + layer_shift.astype(jnp.float32)).astype(jnp.bfloat16)
    causal = jnp.tril(jnp.ones((BLOCK, BLOCK), dtype=bool))
    masked = jnp.where(causal[None], mix_kernel, jnp.zeros_like(mix_kernel))
    blocks = values.reshape(-1, BLOCK, GROUPS, GROUP_CH).astype(jnp.float32)
    mixing = jnp.einsum('gts,nsgc->ntgc', masked.astype(jnp.float32), blocks)
    mixing = mixing + mix_offset.astype(jnp.float32).T[None, :, :, None]
    gated_rows = (gate_u * mixing.reshape(gate_u.shape)).astype(jnp.bfloat16)
    mixer_out = lax.dot_general(gated_rows, out_proj, (((1,), (1,)), ((), ())), preferred_element_type=jnp.float32)
    middle = (tokens.astype(jnp.float32) + mixer_out).astype(jnp.bfloat16)
    normed2 = rms_norm(middle, ffn_gain)
    gate_pre = jnp.dot(normed2, ffn_gate, preferred_element_type=jnp.float32)
    up_pre = jnp.dot(normed2, ffn_up, preferred_element_type=jnp.float32)
    hidden = (jax.nn.silu(gate_pre) * up_pre).astype(jnp.bfloat16)
    run_len = FF // N_TP
    summed = jnp.zeros((tokens.shape[0], D), jnp.float32)
    for run_id in range(N_TP):
        hidden_run = hidden[:, run_id * run_len:(run_id + 1) * run_len]
        weight_run = ffn_down[:, run_id * run_len:(run_id + 1) * run_len]
        partial_value = lax.dot_general(hidden_run, weight_run, (((1,), (1,)), ((), ())), preferred_element_type=jnp.float32)
        summed = summed + partial_value.astype(jnp.bfloat16).astype(jnp.float32)
    return (middle.astype(jnp.float32) + summed).astype(jnp.bfloat16)
```

```python
import functools

import jax
import jax.numpy as jnp
from jax import lax
from jax.experimental import pallas as pl
from jax.experimental.pallas import tpu as pltpu
from jax.sharding import PartitionSpec as P

epsilon = 1e-06
f32, bf16 = jnp.float32, jnp.bfloat16
VMEM_LIMIT = 56 * 1024 * 1024


def xor_permute(x, axis, m, n):
    return lax.ppermute(x, axis, [(i, i ^ m) for i in range(n)])


def bits(n, low=1):
    out = []
    while low < n:
        out.append(low)
        low *= 2
    return out


def absolute(items, me):
    items = list(items)
    for m in bits(len(items)):
        flip = (me & m) != 0
        items = [jnp.where(flip, items[i ^ m], items[i]) for i in range(len(items))]
    return items


def contract_last(left, right):
    return lax.dot_general(left, right, (((1,), (1,)), ((), ())), preferred_element_type=f32)


def mixer_kernel(cfg, place, tok, gain, lgain, lshift, mkern, moff, fgain, *rest):
    bundles, (mid, normed2, wbuf, sem) = rest[: len(cfg["segments"])], rest[len(cfg["segments"]) :]
    k, r, t = place[0], place[1], place[2]
    rows, part, lw, width = cfg["rows"], cfg["part"], cfg["lw"], cfg["width"]
    copies = []
    for ref, segs in zip(bundles, cfg["segments"]):
        for start, count, j, rr, tt in segs:
            base = (k ^ j) * rows
            if rr is not None:
                base = base + (r ^ rr) * part
            copies.append(
                pltpu.make_async_copy(
                    ref.at[pl.ds(start, count)],
                    wbuf.at[tt, pl.ds(pl.multiple_of(base, part), count)],
                    sem.at[len(copies)],
                )
            )
    for c in copies:
        c.start()
    x = tok[...].astype(f32)
    scale = lax.rsqrt(jnp.mean(x * x, axis=-1, keepdims=True) + epsilon)
    normed = (x * scale * gain[...].astype(f32)).astype(bf16)
    for c in copies:
        c.wait()
    n_tp = wbuf.shape[0]
    gate_u, act = [], []
    total = squares = 0.0
    for tt in range(n_tp):
        pre = jnp.dot(normed, wbuf[tt, :, : 2 * lw], preferred_element_type=f32)
        gate_u.append(jax.nn.gelu(pre[:, :lw]))
        a = jax.nn.gelu(pre[:, lw:])
        act.append(a)
        total = total + jnp.sum(a, axis=-1, keepdims=True)
        squares = squares + jnp.sum(a * a, axis=-1, keepdims=True)
    center = total / width
    spread = squares / width - center * center
    inv = lax.rsqrt(spread + epsilon)
    span = mkern.shape[1]
    causal = lax.broadcasted_iota(jnp.int32, (span, span), 0) >= lax.broadcasted_iota(
        jnp.int32, (span, span), 1
    )
    out = None
    for tt in range(n_tp):
        own = t ^ tt
        group = (own * lw) // cfg["group_ch"]
        values = (
            (act[tt] - center) * inv * lgain[own].astype(f32) + lshift[own].astype(f32)
        ).astype(bf16)
        kern = jnp.where(causal, mkern[group].astype(f32), 0.0).astype(bf16)
        offset = moff[group].astype(f32)
        mixed = [
            jnp.dot(kern, values[i : i + span], preferred_element_type=f32) + offset
            for i in range(0, values.shape[0], span)
        ]
        mixed = mixed[0] if len(mixed) == 1 else jnp.concatenate(mixed, axis=0)
        gated = (gate_u[tt] * mixed).astype(bf16)
        term = contract_last(gated, wbuf[tt, :, 2 * lw :])
        out = term if out is None else out + term
    middle = (x + out).astype(bf16)
    mid[...] = middle
    m = middle.astype(f32)
    scale2 = lax.rsqrt(jnp.mean(m * m, axis=-1, keepdims=True) + epsilon)
    normed2[...] = (m * scale2 * fgain[...].astype(f32)).astype(bf16)


def hidden_kernel(cfg, place, *refs):
    n = cfg["tokens"]
    tokens, weights = refs[:n], refs[n : n + len(cfg["weights"])]
    hid, wbuf, sem = refs[n + len(cfg["weights"]) :]
    k, r = place[0], place[1]
    copies = []
    for i, (ref, (j, rr)) in enumerate(zip(weights, cfg["weights"])):
        base = (k ^ j) * cfg["rows"]
        if rr is not None:
            base = base + (r ^ rr) * cfg["part"]
        base = pl.multiple_of(base, cfg["part"])
        copies.append(pltpu.make_async_copy(ref, wbuf.at[pl.ds(base, ref.shape[0])], sem.at[i]))
    for c in copies:
        c.start()
    for c in copies:
        c.wait()
    half = hid.shape[1]
    start = 0
    for ref in tokens:
        pre = jnp.dot(ref[...], wbuf[...], preferred_element_type=f32)
        size = ref.shape[0]
        hid[start : start + size] = (jax.nn.silu(pre[:, :half]) * pre[:, half:]).astype(bf16)
        start += size


def down_kernel(packed, hid, *refs):
    weights, out = refs[:-1], refs[-1]
    half = hid.shape[1]
    col = 0
    h = hid[...]
    for ref in weights:
        for i in range(2 if packed else 1):
            w = ref[:, i * half : (i + 1) * half]
            out[:, col : col + w.shape[0]] = contract_last(h, w).astype(bf16)
            col += w.shape[0]


def per_device(
    sizes,
    tokens,
    mix_gain,
    gate_proj,
    value_proj,
    layer_gain,
    layer_shift,
    mix_kernel,
    mix_offset,
    out_proj,
    ffn_gain,
    ffn_gate,
    ffn_up,
    ffn_down,
):
    n_rep, n_fs, n_tp = sizes
    r, k, t = lax.axis_index("rep"), lax.axis_index("fs"), lax.axis_index("tp")
    b = k & 1
    place = jnp.stack([k, r, t]).astype(jnp.int32)
    count, d_model = tokens.shape
    rows, lw = gate_proj.shape
    part = rows // n_rep
    width = layer_gain.shape[0]
    ff = ffn_gate.shape[1]
    half = ff // 2
    any_spec = pl.BlockSpec(memory_space=pl.ANY)
    vmem_spec = pl.BlockSpec(memory_space=pltpu.VMEM)
    smem_spec = pl.BlockSpec(memory_space=pltpu.SMEM)
    far_first = list(range(n_fs - 1, 0, -1))

    pack = jnp.concatenate([gate_proj, value_proj, out_proj], axis=1)
    mine = lax.dynamic_slice_in_dim(pack, r * part, part, axis=0)
    got = {j: xor_permute(mine, "fs", j, n_fs) for j in range(1, n_fs)}

    def exchange(bundles, axis, m, n):
        arrays, segs, at = [], [], 0
        for array, entries in bundles:
            if axis == "rep":
                entries = [e for e in entries if e[3] is not None]
                if not entries:
                    continue
            if len(entries) == 1 and entries[0][1] != array.shape[0]:
                array = array[entries[0][0] : entries[0][0] + entries[0][1]]
                entries = [(0,) + entries[0][1:]]
            arrays.append(array)
            for start, num, j, rr, tt in entries:
                if axis == "rep":
                    rr = rr ^ m
                else:
                    tt = tt ^ m
                segs.append((start + at, num, j, rr, tt))
            at += array.shape[0]
        joined = arrays[0] if len(arrays) == 1 else jnp.concatenate(arrays, axis=0)
        return (xor_permute(joined, axis, m, n), segs)

    near = [(pack, [(0, rows, 0, None, 0)])]
    near += [(got[j], [(0, part, j, 0, 0)]) for j in range(1, n_fs // 2)]
    far = [(got[j], [(0, part, j, 0, 0)]) for j in range(n_fs // 2, n_fs)]
    steps = [("rep", m, n_rep) for m in bits(n_rep)] + [("tp", m, n_tp) for m in bits(n_tp, 2)]
    for step in steps:
        near.append(exchange(near, *step))
    for step in reversed(steps):
        far.append(exchange(far, *step))
    bundles = near + far
    for bundle in list(bundles):
        for m in bits(min(n_tp, 2)):
            bundles.append(exchange([bundle], "tp", m, n_tp))

    def columns(w, which):
        return jnp.where(which == 0, w[:, :half], w[:, half:])

    def take_part(w, rr):
        return lax.dynamic_slice_in_dim(w, (r ^ rr) * part, part, axis=0)

    gate_up = jnp.concatenate([columns(ffn_gate, b), columns(ffn_up, b)], axis=1)
    g_part, u_part = take_part(ffn_gate, 0), take_part(ffn_up, 0)
    gu_same = jnp.concatenate([columns(g_part, b), columns(u_part, b)], axis=1)
    gu_other = jnp.concatenate([columns(g_part, 1 - b), columns(u_part, 1 - b)], axis=1)
    gu_z = {j: xor_permute(gu_other if j & 1 else gu_same, "fs", j, n_fs) for j in far_first}
    gu_weights, gu_where = [gate_up], [(0, None)]
    for j in far_first:
        gu_weights.append(gu_z[j])
        gu_where.append((j, 0))
        for m in range(1, n_rep):
            gu_weights.append(xor_permute(gu_z[j], "rep", m, n_rep))
            gu_where.append((j, m))

    segments = [segs for _, segs in bundles]
    cfg = dict(
        rows=rows,
        part=part,
        lw=lw,
        width=width,
        group_ch=width // mix_kernel.shape[0],
        segments=segments,
    )
    n_copies = sum(len(s) for s in segments)
    middle, normed2 = pl.pallas_call(
        functools.partial(mixer_kernel, cfg),
        out_shape=[jax.ShapeDtypeStruct((count, d_model), bf16)] * 2,
        in_specs=[smem_spec] + [vmem_spec] * 7 + [any_spec] * len(bundles),
        out_specs=[vmem_spec] * 2,
        scratch_shapes=[
            pltpu.VMEM((n_tp, d_model, 3 * lw), bf16),
            pltpu.SemaphoreType.DMA((n_copies,)),
        ],
        compiler_params=pltpu.CompilerParams(vmem_limit_bytes=VMEM_LIMIT),
        cost_estimate=pl.CostEstimate(
            flops=6 * count * d_model * width,
            bytes_accessed=6 * d_model * width,
            transcendentals=2 * count * width,
        ),
        name="mixer",
    )(
        place,
        tokens,
        mix_gain[None],
        layer_gain.reshape(n_tp, 1, lw),
        layer_shift.reshape(n_tp, 1, lw),
        mix_kernel,
        mix_offset[:, :, None],
        ffn_gain[None],
        *[array for array, _ in bundles],
    )

    ny = n_tp // 2
    h = count // 2
    col_a, col_b = normed2[:h], normed2[h:]
    col_a = jnp.concatenate([col_a, xor_permute(col_a, "fs", 1, n_fs)], axis=0)
    for m in bits(n_tp, 2):
        col_a = jnp.concatenate([col_a, xor_permute(col_a, "tp", m, n_tp)], axis=0)
        col_b = jnp.concatenate([col_b, xor_permute(col_b, "tp", m, n_tp)], axis=0)
    col_b = jnp.concatenate([col_b, xor_permute(col_b, "fs", 1, n_fs)], axis=0)
    groups = [col_a, col_b, xor_permute(col_a, "tp", 1, n_tp), xor_permute(col_b, "tp", 1, n_tp)]
    group_tokens = sum(g.shape[0] for g in groups)

    def fold(w):
        return jnp.concatenate([w[: part // 2], w[part // 2 :]], axis=1)

    down_own = jnp.concatenate([columns(take_part(ffn_down, m), b) for m in range(n_rep)], axis=0)
    d_part = take_part(ffn_down, 0)
    d_same, d_other = fold(columns(d_part, b)), fold(columns(d_part, 1 - b))
    d_same, d_other, _ = lax.optimization_barrier((d_same, d_other, normed2))
    d_z = {j: xor_permute(d_other if j & 1 else d_same, "fs", j, n_fs) for j in far_first}
    d_x = {j: [xor_permute(d_z[j], "rep", m, n_rep) for m in range(1, n_rep)] for j in far_first}

    hidden = pl.pallas_call(
        functools.partial(
            hidden_kernel, dict(rows=rows, part=part, tokens=len(groups), weights=gu_where)
        ),
        out_shape=jax.ShapeDtypeStruct((group_tokens, half), bf16),
        in_specs=[smem_spec] + [vmem_spec] * len(groups) + [any_spec] * len(gu_weights),
        out_specs=vmem_spec,
        scratch_shapes=[
            pltpu.VMEM((d_model, ff), bf16),
            pltpu.SemaphoreType.DMA((len(gu_weights),)),
        ],
        compiler_params=pltpu.CompilerParams(vmem_limit_bytes=VMEM_LIMIT),
        cost_estimate=pl.CostEstimate(
            flops=2 * group_tokens * d_model * ff,
            bytes_accessed=2 * d_model * (group_tokens + ff),
            transcendentals=group_tokens * half,
        ),
        name="hidden",
    )(place, *groups, *gu_weights)

    def down(weights, packed):
        return pl.pallas_call(
            functools.partial(down_kernel, packed),
            out_shape=jax.ShapeDtypeStruct((group_tokens, rows), bf16),
            in_specs=[vmem_spec] * (1 + len(weights)),
            out_specs=vmem_spec,
            compiler_params=pltpu.CompilerParams(vmem_limit_bytes=VMEM_LIMIT),
            cost_estimate=pl.CostEstimate(
                flops=2 * group_tokens * half * rows,
                bytes_accessed=2 * group_tokens * (half + rows),
                transcendentals=0,
            ),
            name="down",
        )(hidden, *weights)

    def add(left, right):
        return (left.astype(f32) + right.astype(f32)).astype(bf16)

    kept, sent = {}, {}
    for j in range(n_fs):
        partial_sum = down([down_own], False) if j == 0 else down([d_z[j]] + d_x[j], True)
        part_tokens = group_tokens // 2
        total = add(partial_sum[:part_tokens], xor_permute(partial_sum[part_tokens:], "tp", 1, n_tp))
        left = total[: part_tokens // 2].reshape(ny, 2, h, rows)
        right = total[part_tokens // 2 :].reshape(2, ny, h, rows)
        for m in reversed(bits(n_tp, 2)):
            n = m // 2
            out_block = jnp.concatenate(
                [left[n:].reshape(-1, rows), right[:, n:].reshape(-1, rows)], axis=0
            )
            back = xor_permute(out_block, "tp", m, n_tp)
            mid_row = back.shape[0] // 2
            left = add(left[:n], back[:mid_row].reshape(n, 2, h, rows))
            right = add(right[:, :n], back[mid_row:].reshape(2, n, h, rows))
        kept[j] = jnp.concatenate([left[0, 0], right[0, 0]], axis=0)
        sent[j] = xor_permute(
            jnp.concatenate([left[0, 1], right[1, 0]], axis=0), "fs", 1, n_fs
        )
    pieces = []
    for j in range(n_fs):
        total = kept[j].astype(f32) + sent[j ^ 1].astype(f32)
        pieces.append(
            jnp.concatenate(
                absolute([total[:, m * part : (m + 1) * part] for m in range(n_rep)], r), axis=1
            )
        )
    summed = jnp.concatenate(absolute(pieces, k), axis=1)
    return (middle.astype(f32) + summed).astype(bf16)


def solution(mesh):
    token_spec = P(("rep", "fs", "tp"), None)
    weight_spec = P("fs", "tp")
    placed = (
        token_spec,
        P(),
        weight_spec,
        weight_spec,
        P(),
        P(),
        P(),
        P(),
        weight_spec,
        P(),
        weight_spec,
        weight_spec,
        weight_spec,
    )
    sizes = (mesh.shape["rep"], mesh.shape["fs"], mesh.shape["tp"])
    return jax.shard_map(
        functools.partial(per_device, sizes),
        mesh=mesh,
        in_specs=placed,
        out_specs=token_spec,
        check_vma=False,
    )
```

```python
import functools

import jax
import jax.numpy as jnp
from jax import lax
from jax.experimental import pallas as pl
from jax.experimental.pallas import tpu as pltpu
from jax.sharding import PartitionSpec as P


epsilon = 1e-06
f32, bf16 = jnp.float32, jnp.bfloat16
MIB = 1024 * 1024


def xor_permute(x, axis, m, n):
    return lax.ppermute(x, axis, [(i, i ^ m) for i in range(n)])


def bits(n, low=1):
    out = []
    while low < n:
        out.append(low)
        low *= 2
    return out


def absolute(items, me):
    items = list(items)
    for m in bits(len(items)):
        flip = (me & m) != 0
        items = [jnp.where(flip, items[i ^ m], items[i]) for i in range(len(items))]
    return items


def contract_last(left, right):
    return lax.dot_general(left, right, (((1,), (1,)), ((), ())), preferred_element_type=f32)


def pack_kernel(part, *refs):
    weights, (full, mine, sem) = refs[:-3], refs[-3:]
    base = pl.multiple_of(lax.axis_index("rep") * part, part)
    copies = []
    for i, ref in enumerate(weights):
        copies.append(
            pltpu.make_async_copy(ref.at[pl.ds(base, part)], mine.at[i], sem.at[len(copies)])
        )
        copies.append(pltpu.make_async_copy(ref, full.at[i], sem.at[len(copies)]))
    for c in copies:
        c.start()
    for c in copies:
        c.wait()


def mixer_kernel(cfg, tok, gain, lgain, lshift, mkern, moff, fgain, *rest):
    bundles, (mid, normed2, wbuf, sem) = rest[: len(cfg["segments"])], rest[len(cfg["segments"]) :]
    k, r, t = lax.axis_index("fs"), lax.axis_index("rep"), lax.axis_index("tp")
    rows, part, lw, width = cfg["rows"], cfg["part"], cfg["lw"], cfg["width"]
    copies = []
    for ref, segs in zip(bundles, cfg["segments"]):
        for start, count, j, rr, tt in segs:
            base = (k ^ j) * rows
            if rr is not None:
                base = base + (r ^ rr) * part
            copies.append(
                pltpu.make_async_copy(
                    ref.at[:, pl.ds(start, count)],
                    wbuf.at[tt, :, pl.ds(pl.multiple_of(base, part), count)],
                    sem.at[len(copies)],
                )
            )
    for c in copies:
        c.start()
    x = tok[...].astype(f32)
    scale = lax.rsqrt(jnp.mean(x * x, axis=-1, keepdims=True) + epsilon)
    normed = (x * scale * gain[...].astype(f32)).astype(bf16)
    for c in copies:
        c.wait()
    n_tp = wbuf.shape[0]
    gate_u, act = [], []
    total = squares = 0.0
    for tt in range(n_tp):
        gate_u.append(jax.nn.gelu(jnp.dot(normed, wbuf[tt, 0], preferred_element_type=f32)))
        a = jax.nn.gelu(jnp.dot(normed, wbuf[tt, 1], preferred_element_type=f32))
        act.append(a)
        total = total + jnp.sum(a, axis=-1, keepdims=True)
        squares = squares + jnp.sum(a * a, axis=-1, keepdims=True)
    center = total / width
    spread = squares / width - center * center
    inv = lax.rsqrt(spread + epsilon)
    span = mkern.shape[1]
    causal = lax.broadcasted_iota(jnp.int32, (span, span), 0) >= lax.broadcasted_iota(
        jnp.int32, (span, span), 1
    )
    diagonal = lax.broadcasted_iota(jnp.int32, (span, span), 0) == lax.broadcasted_iota(
        jnp.int32, (span, span), 1
    )
    out = None
    for tt in range(n_tp):
        own = t ^ tt
        group = (own * lw) // cfg["group_ch"]
        values = (
            (act[tt] - center) * inv * lgain[own].astype(f32) + lshift[own].astype(f32)
        ).astype(bf16)
        kern = jnp.where(causal, mkern[group].astype(f32), 0.0).astype(bf16)
        offset = jnp.sum(jnp.where(diagonal, moff[group].astype(f32), 0.0), axis=1, keepdims=True)
        mixed = [
            jnp.dot(kern, values[i : i + span], preferred_element_type=f32) + offset
            for i in range(0, values.shape[0], span)
        ]
        mixed = mixed[0] if len(mixed) == 1 else jnp.concatenate(mixed, axis=0)
        gated = (gate_u[tt] * mixed).astype(bf16)
        term = contract_last(gated, wbuf[tt, 2])
        out = term if out is None else out + term
    middle = (x + out).astype(bf16)
    mid[...] = middle
    m = middle.astype(f32)
    scale2 = lax.rsqrt(jnp.mean(m * m, axis=-1, keepdims=True) + epsilon)
    normed2[...] = (m * scale2 * fgain[...].astype(f32)).astype(bf16)


def hidden_kernel(cfg, *refs):
    n = cfg["tokens"]
    tokens, weights = refs[:n], refs[n : n + len(cfg["weights"])]
    hid, wbuf, sem = refs[n + len(cfg["weights"]) :]
    k, r = lax.axis_index("fs"), lax.axis_index("rep")
    copies = []
    for i, (ref, (j, rr)) in enumerate(zip(weights, cfg["weights"])):
        base = (k ^ j) * cfg["rows"]
        if rr is not None:
            base = base + (r ^ rr) * cfg["part"]
        base = pl.multiple_of(base, cfg["part"])
        copies.append(pltpu.make_async_copy(ref, wbuf.at[pl.ds(base, ref.shape[0])], sem.at[i]))
    for c in copies:
        c.start()
    for c in copies:
        c.wait()
    half = hid.shape[1]
    start = 0
    for ref in tokens:
        pre = jnp.dot(ref[...], wbuf[...], preferred_element_type=f32)
        size = ref.shape[0]
        hid[start : start + size] = (jax.nn.silu(pre[:, :half]) * pre[:, half:]).astype(bf16)
        start += size


def down_kernel(packed, hid, *refs):
    weights, (keep, send) = refs[:-2], refs[-2:]
    half = hid.shape[1]
    top = keep.shape[0]
    col = 0
    h = hid[...]
    for ref in weights:
        for i in range(2 if packed else 1):
            w = ref[:, i * half : (i + 1) * half]
            res = contract_last(h, w).astype(bf16)
            keep[:, col : col + w.shape[0]] = res[:top]
            send[:, col : col + w.shape[0]] = res[top:]
            col += w.shape[0]


def per_device(
    sizes,
    tokens,
    mix_gain,
    gate_proj,
    value_proj,
    layer_gain,
    layer_shift,
    mix_kernel,
    mix_offset,
    out_proj,
    ffn_gain,
    ffn_gate,
    ffn_up,
    ffn_down,
):
    n_rep, n_fs, n_tp = sizes
    r, k = lax.axis_index("rep"), lax.axis_index("fs")
    b = k & 1
    count, d_model = tokens.shape
    rows, lw = gate_proj.shape
    part = rows // n_rep
    width = layer_gain.shape[0]
    ff = ffn_gate.shape[1]
    half = ff // 2
    any_spec = pl.BlockSpec(memory_space=pl.ANY)
    hbm_spec = pl.BlockSpec(memory_space=pltpu.HBM)
    vmem_spec = pl.BlockSpec(memory_space=pltpu.VMEM)
    far_first = list(range(n_fs - 1, 0, -1))

    pack, mine = pl.pallas_call(
        functools.partial(pack_kernel, part),
        out_shape=[
            jax.ShapeDtypeStruct((3, rows, lw), bf16),
            jax.ShapeDtypeStruct((3, part, lw), bf16),
        ],
        in_specs=[hbm_spec] * 3,
        out_specs=[vmem_spec] * 2,
        scratch_shapes=[pltpu.SemaphoreType.DMA((6,))],
        compiler_params=pltpu.CompilerParams(vmem_limit_bytes=4 * MIB),
        name="pack",
    )(gate_proj, value_proj, out_proj)
    got = {j: xor_permute(mine, "fs", j, n_fs) for j in far_first}

    def columns(w, which):
        return jnp.where(which == 0, w[:, :half], w[:, half:])

    def take_part(w, rr):
        return lax.dynamic_slice_in_dim(w, (r ^ rr) * part, part, axis=0)

    gate_up = jnp.concatenate([columns(ffn_gate, b), columns(ffn_up, b)], axis=1)
    g_part, u_part = take_part(ffn_gate, 0), take_part(ffn_up, 0)
    gu_same = jnp.concatenate([columns(g_part, b), columns(u_part, b)], axis=1)
    gu_other = jnp.concatenate([columns(g_part, 1 - b), columns(u_part, 1 - b)], axis=1)
    gu_z = {j: xor_permute(gu_other if j & 1 else gu_same, "fs", j, n_fs) for j in far_first}
    gu_weights, gu_where = [None], [(0, None)]
    for j in far_first:
        gu_weights.append(gu_z[j])
        gu_where.append((j, 0))
        for m in range(1, n_rep):
            gu_weights.append(xor_permute(gu_z[j], "rep", m, n_rep))
            gu_where.append((j, m))

    def fold(w):
        return jnp.concatenate([w[: part // 2], w[part // 2 :]], axis=1)

    down_own = jnp.concatenate([columns(take_part(ffn_down, m), b) for m in range(n_rep)], axis=0)
    d_part = take_part(ffn_down, 0)
    d_same, d_other = fold(columns(d_part, b)), fold(columns(d_part, 1 - b))

    def exchange(bundles, axis, m, n):
        arrays, segs, at = [], [], 0
        for array, entries in bundles:
            if axis == "rep":
                entries = [e for e in entries if e[3] is not None]
                if not entries:
                    continue
            arrays.append(array)
            for start, num, j, rr, tt in entries:
                if axis == "rep":
                    rr = rr ^ m
                else:
                    tt = tt ^ m
                segs.append((start + at, num, j, rr, tt))
            at += array.shape[1]
        joined = arrays[0] if len(arrays) == 1 else jnp.concatenate(arrays, axis=1)
        return (xor_permute(joined, axis, m, n), segs)

    smalls = (
        mix_gain[None],
        layer_gain.reshape(n_tp, 1, lw),
        layer_shift.reshape(n_tp, 1, lw),
        mix_offset[:, None, :],
        ffn_gain[None],
    )
    tied = lax.optimization_barrier((got[1], smalls, gate_up, down_own, d_same, d_other))
    got[1], smalls, gate_up, down_own, d_same, d_other = tied

    near = [(pack, [(0, rows, 0, None, 0)])]
    near += [(got[j], [(0, part, j, 0, 0)]) for j in range(1, n_fs // 2)]
    far = [(got[j], [(0, part, j, 0, 0)]) for j in range(n_fs // 2, n_fs)]
    steps = [("rep", m, n_rep) for m in bits(n_rep)] + [("tp", m, n_tp) for m in bits(n_tp, 2)]
    for step in steps:
        near.append(exchange(near, *step))
    for step in reversed(steps):
        far.append(exchange(far, *step))
    bundles = near + far
    for bundle in list(bundles):
        bundles.append(exchange([bundle], "tp", 1, n_tp))

    gu_weights[0] = gate_up
    segments = [segs for _, segs in bundles]
    cfg = dict(
        rows=rows,
        part=part,
        lw=lw,
        width=width,
        group_ch=width // mix_kernel.shape[0],
        segments=segments,
    )
    n_copies = sum(len(s) for s in segments)
    middle, normed2 = pl.pallas_call(
        functools.partial(mixer_kernel, cfg),
        out_shape=[jax.ShapeDtypeStruct((count, d_model), bf16)] * 2,
        in_specs=[vmem_spec] * 7 + [any_spec] * len(bundles),
        out_specs=[vmem_spec] * 2,
        scratch_shapes=[
            pltpu.VMEM((n_tp, 3, d_model, lw), bf16),
            pltpu.SemaphoreType.DMA((n_copies,)),
        ],
        compiler_params=pltpu.CompilerParams(vmem_limit_bytes=24 * MIB),
        cost_estimate=pl.CostEstimate(
            flops=6 * count * d_model * width,
            bytes_accessed=6 * d_model * width,
            transcendentals=2 * count * width,
        ),
        name="mixer",
    )(
        tokens,
        *smalls[:3],
        mix_kernel,
        *smalls[3:],
        *[array for array, _ in bundles],
    )

    ny = n_tp // 2
    h = count // 2
    col_a, col_b = normed2[:h], normed2[h:]
    col_a = jnp.concatenate([col_a, xor_permute(col_a, "fs", 1, n_fs)], axis=0)
    for m in bits(n_tp, 2):
        col_a = jnp.concatenate([col_a, xor_permute(col_a, "tp", m, n_tp)], axis=0)
        col_b = jnp.concatenate([col_b, xor_permute(col_b, "tp", m, n_tp)], axis=0)
    col_b = jnp.concatenate([col_b, xor_permute(col_b, "fs", 1, n_fs)], axis=0)
    groups = [col_a, col_b, xor_permute(col_a, "tp", 1, n_tp), xor_permute(col_b, "tp", 1, n_tp)]
    group_tokens = sum(g.shape[0] for g in groups)

    d_z = {j: xor_permute(d_other if j & 1 else d_same, "fs", j, n_fs) for j in far_first}
    d_x = {j: [xor_permute(d_z[j], "rep", m, n_rep) for m in range(1, n_rep)] for j in far_first}

    hidden = pl.pallas_call(
        functools.partial(
            hidden_kernel, dict(rows=rows, part=part, tokens=len(groups), weights=gu_where)
        ),
        out_shape=jax.ShapeDtypeStruct((group_tokens, half), bf16),
        in_specs=[vmem_spec] * len(groups) + [any_spec] * len(gu_weights),
        out_specs=vmem_spec,
        scratch_shapes=[
            pltpu.VMEM((d_model, ff), bf16),
            pltpu.SemaphoreType.DMA((len(gu_weights),)),
        ],
        compiler_params=pltpu.CompilerParams(vmem_limit_bytes=24 * MIB),
        cost_estimate=pl.CostEstimate(
            flops=2 * group_tokens * d_model * ff,
            bytes_accessed=2 * d_model * (group_tokens + ff),
            transcendentals=group_tokens * half,
        ),
        name="hidden",
    )(*groups, *gu_weights)

    def down(weights, packed):
        return pl.pallas_call(
            functools.partial(down_kernel, packed),
            out_shape=[jax.ShapeDtypeStruct((group_tokens // 2, rows), bf16)] * 2,
            in_specs=[vmem_spec] * (1 + len(weights)),
            out_specs=[vmem_spec] * 2,
            compiler_params=pltpu.CompilerParams(vmem_limit_bytes=12 * MIB),
            cost_estimate=pl.CostEstimate(
                flops=2 * group_tokens * half * rows,
                bytes_accessed=2 * group_tokens * (half + rows),
                transcendentals=0,
            ),
        )(hidden, *weights)

    def add(left, right):
        return (left.astype(f32) + right.astype(f32)).astype(bf16)

    kept, sent = {}, {}
    for j in range(n_fs):
        keep, send = down([d_z[j]] + d_x[j] if j else [down_own], j > 0)
        part_tokens = group_tokens // 2
        total = add(keep, xor_permute(send, "tp", 1, n_tp))
        left = total[: part_tokens // 2].reshape(ny, 2, h, rows)
        right = total[part_tokens // 2 :].reshape(2, ny, h, rows)
        for m in reversed(bits(n_tp, 2)):
            n = m // 2
            out_block = jnp.concatenate(
                [left[n:].reshape(-1, rows), right[:, n:].reshape(-1, rows)], axis=0
            )
            back = xor_permute(out_block, "tp", m, n_tp)
            mid_row = back.shape[0] // 2
            left = add(left[:n], back[:mid_row].reshape(n, 2, h, rows))
            right = add(right[:, :n], back[mid_row:].reshape(2, n, h, rows))
        kept[j] = jnp.concatenate([left[0, 0], right[0, 0]], axis=0)
        sent[j] = xor_permute(jnp.concatenate([left[0, 1], right[1, 0]], axis=0), "fs", 1, n_fs)
    pieces = []
    for j in range(n_fs):
        total = kept[j].astype(f32) + sent[j ^ 1].astype(f32)
        pieces.append(
            jnp.concatenate(
                absolute([total[:, m * part : (m + 1) * part] for m in range(n_rep)], r), axis=1
            )
        )
    summed = jnp.concatenate(absolute(pieces, k), axis=1)
    return (middle.astype(f32) + summed).astype(bf16)


def solution(mesh):
    token_spec = P(("rep", "fs", "tp"), None)
    weight_spec = P("fs", "tp")
    placed = (
        token_spec,
        P(),
        weight_spec,
        weight_spec,
        P(),
        P(),
        P(),
        P(),
        weight_spec,
        P(),
        weight_spec,
        weight_spec,
        weight_spec,
    )
    sizes = (mesh.shape["rep"], mesh.shape["fs"], mesh.shape["tp"])

    def body(*args):
        return per_device(sizes, *args)

    return jax.shard_map(
        body, mesh=mesh, in_specs=placed, out_specs=token_spec, check_vma=False
    )
```

```python
import functools

import jax
import jax.numpy as jnp
from jax import lax
from jax.experimental import pallas as pl
from jax.experimental.pallas import tpu as pltpu
from jax.sharding import PartitionSpec as P


epsilon = 1e-06
f32, bf16 = jnp.float32, jnp.bfloat16
MIB = 1024 * 1024


def xor_permute(x, axis, m, n):
    return lax.ppermute(x, axis, [(i, i ^ m) for i in range(n)])


def bits(n, low=1):
    out = []
    while low < n:
        out.append(low)
        low *= 2
    return out


def absolute(items, me):
    items = list(items)
    for m in bits(len(items)):
        flip = (me & m) != 0
        items = [jnp.where(flip, items[i ^ m], items[i]) for i in range(len(items))]
    return items


def contract_last(left, right):
    return lax.dot_general(left, right, (((1,), (1,)), ((), ())), preferred_element_type=f32)


def pack_kernel(part, *refs):
    weights, (full, mine, sem) = refs[:-3], refs[-3:]
    base = pl.multiple_of(lax.axis_index("rep") * part, part)
    copies = []
    for i, ref in enumerate(weights):
        copies.append(
            pltpu.make_async_copy(ref.at[pl.ds(base, part)], mine.at[i], sem.at[len(copies)])
        )
        copies.append(pltpu.make_async_copy(ref, full.at[i], sem.at[len(copies)]))
    for c in copies:
        c.start()
    for c in copies:
        c.wait()


def fetch(pairs, sem):
    copies = [pltpu.make_async_copy(a, b, sem.at[i]) for i, (a, b) in enumerate(pairs)]
    for c in copies:
        c.start()
    for c in copies:
        c.wait()


def send_kernel(part, gate, up, same, other, g, u, sem):
    at = pl.ds(pl.multiple_of(lax.axis_index("rep") * part, part), part)
    fetch([(gate.at[at], g), (up.at[at], u)], sem)
    half = gate.shape[1] // 2
    b = lax.axis_index("fs") & 1
    for case in range(2):

        @pl.when(b == case)
        def _():
            for ref, side in ((same, case), (other, 1 - case)):
                cut = slice(side * half, (side + 1) * half)
                ref[...] = jnp.concatenate([g[:, cut], u[:, cut]], axis=1)


def own_kernel(part, n_rep, gate, up, down, gate_up, down_own, d_same, d_other, g, u, d, sem):
    r = lax.axis_index("rep")
    pairs = [(gate, g), (up, u)]
    for m in range(n_rep):
        at = pl.ds(pl.multiple_of((r ^ m) * part, part), part)
        pairs.append((down.at[at], d.at[pl.ds(m * part, part)]))
    fetch(pairs, sem)
    half = gate.shape[1] // 2
    b = lax.axis_index("fs") & 1
    for case in range(2):

        @pl.when(b == case)
        def _():
            cut = slice(case * half, (case + 1) * half)
            gate_up[...] = jnp.concatenate([g[:, cut], u[:, cut]], axis=1)
            down_own[...] = d[:, cut]
            for ref, side in ((d_same, case), (d_other, 1 - case)):
                cut = slice(side * half, (side + 1) * half)
                ref[...] = jnp.concatenate([d[: part // 2, cut], d[part // 2 : part, cut]], axis=1)


def copy_kernel(x, out):
    out[...] = x[...]


def add_kernel(left, right, keep, send):
    total = (left[...].astype(f32) + right[...].astype(f32)).astype(bf16)
    cut = keep.shape[0]
    keep[...] = total[:cut]
    send[...] = total[cut:]


def rms_norm(x, gain):
    scale = lax.rsqrt(jnp.mean(x * x, axis=-1, keepdims=True) + epsilon)
    return (x * scale * gain).astype(bf16)


def mixer_kernel(cfg, tok_a, tok_b, gain, lgain, lshift, mkern, moff, fgain, *rest):
    bundles, (mid, normed2, wbuf, sem) = rest[: len(cfg["segments"])], rest[len(cfg["segments"]) :]
    k, r, t = lax.axis_index("fs"), lax.axis_index("rep"), lax.axis_index("tp")
    rows, part, lw, width = cfg["rows"], cfg["part"], cfg["lw"], cfg["width"]
    wide, n_tp, ny = cfg["wide"], cfg["n_tp"], cfg["n_tp"] // 2
    copies = []
    for ref, segs in zip(bundles, cfg["segments"]):
        for start, count, j, rr, tt in segs:
            base = (k ^ j) * rows
            if rr is not None:
                base = base + (r ^ rr) * part
            to = pl.ds(pl.multiple_of(base, part), count)
            for m in range(3):
                if wide:
                    place = wbuf.at[to, pl.ds(m * width + tt * lw, lw)]
                else:
                    place = wbuf.at[m * n_tp + tt, to]
                source = ref.at[m, pl.ds(start, count)]
                copies.append(pltpu.make_async_copy(source, place, sem.at[len(copies)]))
    for c in copies:
        c.start()
    h = tok_a.shape[0] // (2 * ny)
    span = mkern.shape[1]
    row = lax.broadcasted_iota(jnp.int32, (span, span), 0)
    col = lax.broadcasted_iota(jnp.int32, (span, span), 1)
    kerns, offsets = [], []
    for tt in range(n_tp):
        group = ((t ^ tt) * lw) // cfg["group_ch"]
        kerns.append(jnp.where(row >= col, mkern[group].astype(f32), 0.0).astype(bf16))
        offset = jnp.where(row == col, moff[group].astype(f32), 0.0)
        offsets.append(jnp.sum(offset, axis=1, keepdims=True))

    def block(i):
        yy, bb = i // 2, i % 2
        at_a, at_b = (yy * 2 + bb) * h, (bb * ny + yy) * h
        return [tok_a[at_a : at_a + h].astype(f32), tok_b[at_b : at_b + h].astype(f32)]

    def project(rows_in, m, tt):
        w = wbuf[:, m * width + tt * lw : m * width + (tt + 1) * lw] if wide else wbuf[m * n_tp + tt]
        return jnp.dot(rows_in, w, preferred_element_type=f32)

    waited = False
    for at in range(0, 2 * ny, 2):
        x = jnp.concatenate(block(at) + block(at + 1), axis=0)
        normed = rms_norm(x, gain[...].astype(f32))
        if not waited:
            for c in copies:
                c.wait()
            waited = True
        gate_u, act = [], []
        total = squares = 0.0
        if wide:
            pre = jnp.dot(normed, wbuf[:, : 2 * width], preferred_element_type=f32)
        for tt in range(n_tp):
            if wide:
                g = pre[:, tt * lw : (tt + 1) * lw]
                v = pre[:, width + tt * lw : width + (tt + 1) * lw]
            else:
                g, v = project(normed, 0, tt), project(normed, 1, tt)
            gate_u.append(jax.nn.gelu(g))
            a = jax.nn.gelu(v)
            act.append(a)
            total = total + jnp.sum(a, axis=-1, keepdims=True)
            squares = squares + jnp.sum(a * a, axis=-1, keepdims=True)
        center = total / width
        spread = squares / width - center * center
        inv = lax.rsqrt(spread + epsilon)
        gated, out = [], None
        for tt in range(n_tp):
            own = t ^ tt
            values = (
                (act[tt] - center) * inv * lgain[own].astype(f32) + lshift[own].astype(f32)
            ).astype(bf16)
            mixed = [
                jnp.dot(kerns[tt], values[i : i + span], preferred_element_type=f32) + offsets[tt]
                for i in range(0, values.shape[0], span)
            ]
            gated.append((gate_u[tt] * jnp.concatenate(mixed, axis=0)).astype(bf16))
            if not wide:
                term = contract_last(gated[tt], wbuf[2 * n_tp + tt])
                out = term if out is None else out + term
        if wide:
            out = contract_last(jnp.concatenate(gated, axis=1), wbuf[:, 2 * width :])
        middle = (x + out).astype(bf16)
        if at == 0:
            mid[...] = middle[: 2 * h]
        normed2[at * 2 * h : (at + 2) * 2 * h] = rms_norm(middle.astype(f32), fgain[...].astype(f32))


def hidden_kernel(cfg, *refs):
    final, blocks, where = cfg["final"], cfg["blocks"], cfg["where"]
    tokens, refs = refs[:2], refs[2:]
    if final:
        base, refs = refs[0], refs[1:]
    weights, (out, wbuf, sem) = refs[: len(where)], refs[len(where) :]
    rows, part = cfg["rows"], cfg["part"]
    k, r = lax.axis_index("fs"), lax.axis_index("rep")
    pairs = []
    for ref, (j, rr) in zip(weights, where):
        at = blocks.index(j) * rows
        if rr is not None:
            at = pl.multiple_of(at + (r ^ rr) * part, part)
        pairs.append((ref, wbuf.at[pl.ds(at, ref.shape[0])]))
    fetch(pairs, sem)
    half = out.shape[1] if final else out.shape[1] // 2
    start = 0
    for ref in tokens:
        for at in range(0, ref.shape[0], cfg["tile"]):
            here = pl.ds(start + at, cfg["tile"])
            pre = base[here] if final else None
            for i, j in enumerate(blocks):
                cols = pl.ds(pl.multiple_of((k ^ j) * rows, rows), rows)
                term = jnp.dot(
                    ref[pl.ds(at, cfg["tile"]), cols],
                    wbuf[i * rows : (i + 1) * rows],
                    preferred_element_type=f32,
                )
                pre = term if pre is None else pre + term
            if final:
                out[here] = (jax.nn.silu(pre[:, :half]) * pre[:, half:]).astype(bf16)
            else:
                out[here] = pre
        start += ref.shape[0]


def down_kernel(packed, hid, *refs):
    weights, (keep, send) = refs[:-2], refs[-2:]
    half = hid.shape[1]
    top = keep.shape[0]
    col = 0
    h = hid[...]
    for ref in weights:
        for i in range(2 if packed else 1):
            w = ref[:, i * half : (i + 1) * half]
            res = contract_last(h, w).astype(bf16)
            keep[:, col : col + w.shape[0]] = res[:top]
            send[:, col : col + w.shape[0]] = res[top:]
            col += w.shape[0]


def per_device(
    sizes,
    tokens,
    mix_gain,
    gate_proj,
    value_proj,
    layer_gain,
    layer_shift,
    mix_kernel,
    mix_offset,
    out_proj,
    ffn_gain,
    ffn_gate,
    ffn_up,
    ffn_down,
):
    n_rep, n_fs, n_tp = sizes
    r, k = lax.axis_index("rep"), lax.axis_index("fs")
    count, d_model = tokens.shape
    rows, lw = gate_proj.shape
    part = rows // n_rep
    width = layer_gain.shape[0]
    ff = ffn_gate.shape[1]
    half = ff // 2
    any_spec = pl.BlockSpec(memory_space=pl.ANY)
    hbm_spec = pl.BlockSpec(memory_space=pltpu.HBM)
    vmem_spec = pl.BlockSpec(memory_space=pltpu.VMEM)
    far_first = list(range(n_fs - 1, 0, -1))

    h = count // 2
    col_a, col_b = tokens[:h], tokens[h:]
    col_a = jnp.concatenate([col_a, xor_permute(col_a, "fs", 1, n_fs)], axis=0)
    for m in bits(n_tp, 2):
        col_a = jnp.concatenate([col_a, xor_permute(col_a, "tp", m, n_tp)], axis=0)
        col_b = jnp.concatenate([col_b, xor_permute(col_b, "tp", m, n_tp)], axis=0)
    col_b = jnp.concatenate([col_b, xor_permute(col_b, "fs", 1, n_fs)], axis=0)

    pack, mine = pl.pallas_call(
        functools.partial(pack_kernel, part),
        out_shape=[
            jax.ShapeDtypeStruct((3, rows, lw), bf16),
            jax.ShapeDtypeStruct((3, part, lw), bf16),
        ],
        in_specs=[hbm_spec] * 3,
        out_specs=[vmem_spec] * 2,
        scratch_shapes=[pltpu.SemaphoreType.DMA((6,))],
        compiler_params=pltpu.CompilerParams(vmem_limit_bytes=4 * MIB),
        name="pack",
    )(gate_proj, value_proj, out_proj)
    got = {j: xor_permute(mine, "fs", j, n_fs) for j in far_first}

    gu_same, gu_other = pl.pallas_call(
        functools.partial(send_kernel, part),
        out_shape=[jax.ShapeDtypeStruct((part, ff), bf16)] * 2,
        in_specs=[any_spec] * 2,
        out_specs=[vmem_spec] * 2,
        scratch_shapes=[pltpu.VMEM((part, ff), bf16)] * 2 + [pltpu.SemaphoreType.DMA((2,))],
        compiler_params=pltpu.CompilerParams(vmem_limit_bytes=8 * MIB),
        cost_estimate=pl.CostEstimate(flops=0, bytes_accessed=8 * part * ff, transcendentals=0),
        name="prepsend",
    )(ffn_gate, ffn_up)
    gu_z = {j: xor_permute(gu_other if j & 1 else gu_same, "fs", j, n_fs) for j in far_first}
    gu_weights, gu_where = [None], [(0, None)]
    for j in far_first:
        gu_weights.append(gu_z[j])
        gu_where.append((j, 0))
        for m in range(1, n_rep):
            gu_weights.append(xor_permute(gu_z[j], "rep", m, n_rep))
            gu_where.append((j, m))

    gate_up, down_own, d_same, d_other = pl.pallas_call(
        functools.partial(own_kernel, part, n_rep),
        out_shape=[
            jax.ShapeDtypeStruct((rows, ff), bf16),
            jax.ShapeDtypeStruct((rows, half), bf16),
            jax.ShapeDtypeStruct((part // 2, ff), bf16),
            jax.ShapeDtypeStruct((part // 2, ff), bf16),
        ],
        in_specs=[any_spec] * 3,
        out_specs=[vmem_spec] * 4,
        scratch_shapes=[pltpu.VMEM((rows, ff), bf16)] * 3
        + [pltpu.SemaphoreType.DMA((2 + n_rep,))],
        compiler_params=pltpu.CompilerParams(vmem_limit_bytes=16 * MIB),
        cost_estimate=pl.CostEstimate(flops=0, bytes_accessed=12 * rows * ff, transcendentals=0),
        name="prepown",
    )(ffn_gate, ffn_up, ffn_down)

    def exchange(bundles, axis, m, n):
        arrays, segs, at = [], [], 0
        for array, entries in bundles:
            if axis == "rep":
                entries = [e for e in entries if e[3] is not None]
                if not entries:
                    continue
            arrays.append(array)
            for start, num, j, rr, tt in entries:
                if axis == "rep":
                    rr = rr ^ m
                else:
                    tt = tt ^ m
                segs.append((start + at, num, j, rr, tt))
            at += array.shape[1]
        joined = arrays[0] if len(arrays) == 1 else jnp.concatenate(arrays, axis=1)
        return (xor_permute(joined, axis, m, n), segs)

    smalls = (
        mix_gain[None],
        layer_gain.reshape(n_tp, 1, lw),
        layer_shift.reshape(n_tp, 1, lw),
        mix_offset[:, None, :],
        ffn_gain[None],
    )
    got[1], smalls = lax.optimization_barrier((got[1], smalls))
    gain = pl.pallas_call(
        copy_kernel,
        out_shape=jax.ShapeDtypeStruct(smalls[0].shape, bf16),
        in_specs=[vmem_spec],
        out_specs=vmem_spec,
        compiler_params=pltpu.CompilerParams(vmem_limit_bytes=1 * MIB),
        cost_estimate=pl.CostEstimate(flops=2048, bytes_accessed=8192, transcendentals=0),
        name="mark",
    )(smalls[0])
    smalls = (gain,) + smalls[1:]

    near = [(pack, [(0, rows, 0, None, 0)])]
    near += [(got[j], [(0, part, j, 0, 0)]) for j in range(1, n_fs // 2)]
    far = [(got[j], [(0, part, j, 0, 0)]) for j in range(n_fs // 2, n_fs)]
    steps = [("rep", m, n_rep) for m in bits(n_rep)] + [("tp", m, n_tp) for m in bits(n_tp, 2)]
    for step in steps:
        near.append(exchange(near, *step))
    for step in reversed(steps):
        far.append(exchange(far, *step))
    bundles = near + far
    for bundle in list(bundles):
        bundles.append(exchange([bundle], "tp", 1, n_tp))

    gu_weights[0] = gate_up
    segments = [segs for _, segs in bundles]
    cfg = dict(
        rows=rows,
        part=part,
        lw=lw,
        width=width,
        group_ch=width // mix_kernel.shape[0],
        segments=segments,
    )
    n_copies = 3 * sum(len(s) for s in segments)
    wide = lw % 128 == 0
    core_tokens = col_a.shape[0] + col_b.shape[0]
    cfg.update(wide=wide, n_tp=n_tp)
    middle, normed2 = pl.pallas_call(
        functools.partial(mixer_kernel, cfg),
        out_shape=[
            jax.ShapeDtypeStruct((count, d_model), bf16),
            jax.ShapeDtypeStruct((core_tokens, d_model), bf16),
        ],
        in_specs=[vmem_spec] * 8 + [any_spec] * len(bundles),
        out_specs=[vmem_spec] * 2,
        scratch_shapes=[
            pltpu.VMEM((d_model, 3 * width) if wide else (3 * n_tp, d_model, lw), bf16),
            pltpu.SemaphoreType.DMA((n_copies,)),
        ],
        compiler_params=pltpu.CompilerParams(vmem_limit_bytes=32 * MIB),
        cost_estimate=pl.CostEstimate(
            flops=6 * core_tokens * d_model * width,
            bytes_accessed=6 * d_model * width,
            transcendentals=2 * core_tokens * width,
        ),
        name="mixer",
    )(
        col_a,
        col_b,
        *smalls[:3],
        mix_kernel,
        *smalls[3:],
        *[array for array, _ in bundles],
    )

    groups = [normed2, xor_permute(normed2, "tp", 1, n_tp)]
    group_tokens = sum(g.shape[0] for g in groups)

    d_z = {j: xor_permute(d_other if j & 1 else d_same, "fs", j, n_fs) for j in far_first}
    d_x = {j: [xor_permute(d_z[j], "rep", m, n_rep) for m in range(1, n_rep)] for j in far_first}

    last = n_fs // 2

    def hidden_call(final, blocks, extra):
        chosen = [(w, p) for w, p in zip(gu_weights, gu_where) if p[0] in blocks]
        width_out, kind = (half, bf16) if final else (ff, f32)
        return pl.pallas_call(
            functools.partial(
                hidden_kernel,
                dict(
                    rows=rows,
                    part=part,
                    final=final,
                    blocks=blocks,
                    where=[p for _, p in chosen],
                    tile=min(256, core_tokens),
                ),
            ),
            out_shape=jax.ShapeDtypeStruct((group_tokens, width_out), kind),
            in_specs=[vmem_spec] * (2 + len(extra)) + [any_spec] * len(chosen),
            out_specs=vmem_spec,
            scratch_shapes=[
                pltpu.VMEM((rows * len(blocks), ff), bf16),
                pltpu.SemaphoreType.DMA((len(chosen),)),
            ],
            compiler_params=pltpu.CompilerParams(vmem_limit_bytes=24 * MIB),
            cost_estimate=pl.CostEstimate(
                flops=2 * group_tokens * rows * len(blocks) * ff,
                bytes_accessed=2 * d_model * group_tokens,
                transcendentals=group_tokens * half,
            ),
        )(*groups, *extra, *[w for w, _ in chosen])

    first_blocks = [j for j in range(n_fs) if j != last]
    begun = hidden_call(False, first_blocks, [])
    hidden = hidden_call(True, [last], [begun])

    def down(weights, packed):
        return pl.pallas_call(
            functools.partial(down_kernel, packed),
            out_shape=[jax.ShapeDtypeStruct((group_tokens // 2, rows), bf16)] * 2,
            in_specs=[vmem_spec] * (1 + len(weights)),
            out_specs=[vmem_spec] * 2,
            compiler_params=pltpu.CompilerParams(vmem_limit_bytes=12 * MIB),
            cost_estimate=pl.CostEstimate(
                flops=2 * group_tokens * half * rows,
                bytes_accessed=2 * group_tokens * (half + rows),
                transcendentals=0,
            ),
        )(hidden, *weights)

    def add(left, right):
        cut = left.shape[0] // 2
        return pl.pallas_call(
            add_kernel,
            out_shape=[jax.ShapeDtypeStruct((cut, left.shape[1]), bf16)] * 2,
            in_specs=[vmem_spec] * 2,
            out_specs=[vmem_spec] * 2,
            compiler_params=pltpu.CompilerParams(vmem_limit_bytes=6 * MIB),
            cost_estimate=pl.CostEstimate(
                flops=left.size, bytes_accessed=8 * left.size, transcendentals=0
            ),
        )(left, right)

    kept, sent = {}, {}
    for j in range(n_fs):
        keep, send = down([d_z[j]] + d_x[j] if j else [down_own], j > 0)
        keep, send = add(keep, xor_permute(send, "tp", 1, n_tp))
        for m in reversed(bits(n_tp, 2)):
            keep, send = add(keep, xor_permute(send, "tp", m, n_tp))
        kept[j] = keep
        sent[j] = xor_permute(send, "fs", 1, n_fs)
    pieces = []
    for j in range(n_fs):
        total = kept[j].astype(f32) + sent[j ^ 1].astype(f32)
        pieces.append(
            jnp.concatenate(
                absolute([total[:, m * part : (m + 1) * part] for m in range(n_rep)], r), axis=1
            )
        )
    summed = jnp.concatenate(absolute(pieces, k), axis=1)
    return (middle.astype(f32) + summed).astype(bf16)


def solution(mesh):
    token_spec = P(("rep", "fs", "tp"), None)
    weight_spec = P("fs", "tp")
    placed = (
        token_spec,
        P(),
        weight_spec,
        weight_spec,
        P(),
        P(),
        P(),
        P(),
        weight_spec,
        P(),
        weight_spec,
        weight_spec,
        weight_spec,
    )
    sizes = (mesh.shape["rep"], mesh.shape["fs"], mesh.shape["tp"])

    def body(*args):
        return per_device(sizes, *args)

    return jax.shard_map(
        body, mesh=mesh, in_specs=placed, out_specs=token_spec, check_vma=False
    )
```
